512 devices in a mesh: ep: 32 (over z, x), tp: 16 (over y, core).
Axes of the slice: x: 4, y: 8, z: 8, core: 2. Of those that a mesh axis runs over, the one named last changes fastest.
Arguments:
- tokens: bfloat16 [256, 4096], P('ep', 'tp'), may hold values from -6 to 6
- norm_gain: float32 [4096], replicated, may hold values from 0.1 to 1.9
- route_experts: int32 [256, 2], P('ep'), may hold values from 0 to 63, all different within a row; in each aligned block of 8 rows (0 to 7, 8 to 15, ...) at most 2 rows name the same one
- route_logits: float32 [256, 2], P('ep'), may hold values from -4 to 4
- expert_gate: bfloat16 [64, 4096, 1024], P('ep', None, 'tp'), may hold values from -0.09375 to 0.09375
- expert_up: bfloat16 [64, 4096, 1024], P('ep', None, 'tp'), may hold values from -0.09375 to 0.09375
- expert_down: bfloat16 [64, 1024, 4096], P('ep', 'tp'), may hold values from -0.1875 to 0.1875
- dense_gate: bfloat16 [4096, 1024], P(None, 'tp'), may hold values from -0.09375 to 0.09375
- dense_up: bfloat16 [4096, 1024], P(None, 'tp'), may hold values from -0.09375 to 0.09375
- dense_down: bfloat16 [1024, 4096], P('tp'), may hold values from -0.1875 to 0.1875
- mix_weight: float32 [4096], replicated, may hold values from -0.09375 to 0.09375
- out_gain: float32 [4096], P('tp'), may hold values from 0.1 to 1.9
Outputs:
- result: bfloat16 [256, 4096], P('ep', 'tp')
The draws below stay inside these ranges and needn't reach their ends.
Inputs may be any that keep to these rules, and one draw needn't show every extreme that they name: `route_experts`: each row names 2 different experts; the 8 rows of one index of ep (aligned blocks) name any one expert at most 2 times, and some block names some expert exactly 2 times; every expert is named somewhere.
All inputs are finite; a program needn't handle non-finite values.
Results may differ from the reference program's by a relative error of at most 0.0025.
Values may be sent and summed in bfloat16 or wider, within the bound.
A program may use at most 64 MiB of HBM per device.

```python
import math
import jax
import jax.numpy as jnp
import numpy as np
from jax import lax

D = 4096
FFE = 1024
DENSE_FF = 1024
TOP = 2
CAP = 2
TOK_DEV = 8
EXPERTS = 64
TOKENS = 256
N_EP = 32


def levels(rng, dims, pieces, low, high):
    level = 1.0
    for dim, shards_of in pieces:
        draws = jax.random.uniform(jax.random.fold_in(jax.random.fold_in(rng, 6), dim), (shards_of,), jnp.float32, low / len(pieces), high / len(pieces))
        level = level * jnp.repeat(jnp.exp(draws), dims[dim] // shards_of).reshape((-1,) + (1,) * (len(dims) - 1 - dim))
    return level


def shared_out(key, own, number, rows, amount, top, reach, lean):
    sequence = jax.random.permutation(key, amount)
    crowded, usual = load_shares(amount, rows * top, reach, lean, True), load_shares(amount, rows * top, reach, lean, False)
    places = jnp.arange(amount)

    def named(tallies, offset_by):
        used = int((tallies > 0).sum())
        fixed = max(1, used // 4)
        shifted = fixed + (places - fixed + offset_by * (used - fixed)) % max(1, amount - fixed)
        return jnp.zeros((amount,), jnp.int32).at[sequence[jnp.where(places < fixed, places, shifted)]].set(jnp.asarray(tallies, jnp.int32))

    tallies = jnp.where(number % 4 == 0, named(crowded, number // 4), named(usual, number - number // 4 - 1))
    mixed = jax.random.permutation(jax.random.fold_in(own, 3), amount)
    donor, taker = mixed[0:amount // 2 * 2:2], mixed[1:amount // 2 * 2:2]
    margin = jnp.minimum(tallies[donor] - 1, reach - tallies[taker]) // 2
    margin = jnp.where((donor == sequence[0]) | (taker == sequence[0]) | (tallies[taker] == 0), 0, jnp.maximum(margin, 0))
    shifted = jax.random.randint(jax.random.fold_in(own, 4), (amount // 2,), 0, 1 << 20) % (margin + 1)
    tallies = tallies.at[donor].add(-shifted).at[taker].add(shifted)
    items = jnp.searchsorted(jnp.cumsum(tallies), jnp.arange(rows * top), side="right").astype(jnp.int32)
    table = items.reshape(top, rows).T
    table = table[jax.random.permutation(jax.random.fold_in(own, 1), rows)]
    offset_by = jax.random.randint(jax.random.fold_in(own, 2), (rows, 1), 0, top)
    return jnp.take_along_axis(table, (jnp.arange(top)[None, :] + offset_by) % top, axis=1)


def load_shares(number_of, total, reach, slope, full):
    loads = [(1 << 20) // math.isqrt(grade ** slope) + 1 for grade in range(1, number_of + 1)]
    largest = reach if full else min(reach, max(-(-total // number_of), total * loads[0] // sum(loads)))
    least = 1 if total - largest >= number_of - 1 else 0
    holding, surplus = [largest] + [least] * (number_of - 1), total - largest - least * (number_of - 1)
    while surplus > 0:
        free = [i for i in range(1, number_of) if holding[i] < largest] or [i for i in range(1, number_of) if holding[i] < reach]
        mass, remaining = sum([loads[i] for i in free]), surplus
        for i in free:
            addition = min(reach - holding[i], max(1, remaining * loads[i] // mass), surplus)
            holding[i] = holding[i] + addition
            surplus = surplus - addition
    return np.array(holding)


def centred(rng, dims, scale, limit, shards=(), held_as=jnp.bfloat16):
    result = jax.random.normal(rng, dims, jnp.float32) * scale
    if len(shards) > 0:
        result = levels(rng, dims, shards, -0.22, 0.18) * result
    return jnp.clip(result, min=-limit, max=limit).astype(held_as)


def setup_inputs(seed: int = 0) -> dict:
    seeds = jax.random.split(jax.random.key(seed), 13)
    tokens = centred(seeds[0], (TOKENS, D), 1.0, 6.0, ((0, 32), (1, 16)))
    norm_gain = jnp.clip(1.0 + 0.18 * jax.random.normal(seeds[1], (D,), jnp.float32), 0.1, 1.9)
    route_experts_keys = jax.random.split(jax.random.fold_in(seeds[2], 1), TOKENS // TOK_DEV)
    route_experts_turns = jax.random.permutation(jax.random.fold_in(seeds[2], 3), TOKENS // TOK_DEV)
    route_experts = jax.vmap(lambda own, number: shared_out(jax.random.fold_in(seeds[2], 2), own, number, TOK_DEV, EXPERTS, TOP, CAP, 2))(route_experts_keys, route_experts_turns).reshape((TOKENS, TOP))
    route_logits = centred(seeds[3], (TOKENS, TOP), 1.0, 4.0, ((0, 32),), jnp.float32)
    expert_gate = centred(seeds[4], (EXPERTS, D, FFE), D ** -0.5, 0.09375, ((0, 32), (2, 16)))
    expert_up = centred(seeds[5], (EXPERTS, D, FFE), D ** -0.5, 0.09375, ((0, 32), (2, 16)))
    expert_down = centred(seeds[6], (EXPERTS, FFE, D), FFE ** -0.5, 0.1875, ((0, 32), (1, 16)))
    dense_gate = centred(seeds[7], (D, DENSE_FF), D ** -0.5, 0.09375, ((1, 16),))
    dense_up = centred(seeds[8], (D, DENSE_FF), D ** -0.5, 0.09375, ((1, 16),))
    dense_down = centred(seeds[9], (DENSE_FF, D), DENSE_FF ** -0.5, 0.1875, ((0, 16),))
    mix_weight = centred(seeds[10], (D,), D ** -0.5, 0.09375, (), jnp.float32)
    out_gain = jnp.clip(1.0 + 0.18 * jax.random.normal(seeds[11], (D,), jnp.float32), 0.1, 1.9)
    return dict(tokens=tokens, norm_gain=norm_gain, route_experts=route_experts, route_logits=route_logits, expert_gate=expert_gate, expert_up=expert_up, expert_down=expert_down, dense_gate=dense_gate, dense_up=dense_up, dense_down=dense_down, mix_weight=mix_weight, out_gain=out_gain)


norm_eps = 1e-06

def reference(tokens, norm_gain, route_experts, route_logits, expert_gate, expert_up, expert_down, dense_gate, dense_up, dense_down, mix_weight, out_gain):
    values = tokens.astype(jnp.float32)
    normed = (values * lax.rsqrt(lax.optimization_barrier(jnp.mean(values * values, axis=1, keepdims=True)) + norm_eps) * norm_gain).astype(jnp.bfloat16)
    weights = jax.nn.softmax(route_logits, axis=-1)
    rows_cap = N_EP * CAP

    def per_expert(running, expert):
        route_hits = route_experts == expert
        routed = jnp.any(route_hits, axis=1)
        row_index = jnp.nonzero(routed, size=rows_cap, fill_value=0)[0].astype(jnp.int32)
        row_count = jnp.sum(routed.astype(jnp.int32))
        usable = (jnp.arange(rows_cap, dtype=jnp.int32) < row_count).astype(jnp.float32)
        picked = normed[row_index]
        gate_act = jnp.dot(picked, expert_gate[expert], preferred_element_type=jnp.float32)
        up_act = jnp.dot(picked, expert_up[expert], preferred_element_type=jnp.float32)
        hidden = (jax.nn.silu(gate_act) * up_act).astype(jnp.bfloat16)
        produced = jnp.dot(hidden, expert_down[expert], preferred_element_type=jnp.float32)
        factor = lax.optimization_barrier(jnp.sum(jnp.where(route_hits, weights, jnp.zeros_like(weights)), axis=1))[row_index] * usable
        return (running.at[row_index].add(factor[:, None] * produced), None)
    expert_mix, _ = lax.scan(per_expert, jnp.zeros((TOKENS, D), jnp.float32), jnp.arange(EXPERTS, dtype=jnp.int32))
    dense_hidden = (jax.nn.silu(jnp.dot(normed, dense_gate, preferred_element_type=jnp.float32)) * jnp.dot(normed, dense_up, preferred_element_type=jnp.float32)).astype(jnp.bfloat16)
    dense_out = jnp.dot(dense_hidden, dense_down, preferred_element_type=jnp.float32)
    mix_gate = jax.nn.sigmoid(jnp.dot(normed.astype(jnp.float32), mix_weight, precision=lax.Precision.HIGHEST))
    combined = expert_mix + mix_gate[:, None] * dense_out
    scaled = combined * lax.rsqrt(lax.optimization_barrier(jnp.mean(combined * combined, axis=1, keepdims=True)) + norm_eps) * out_gain
    return scaled.astype(jnp.bfloat16)
```

```python
import functools

import jax
import jax.numpy as jnp
from jax import lax
from jax.experimental import pallas as pl
from jax.experimental.pallas import tpu as pltpu
from jax.sharding import PartitionSpec as P

MESH = pl.DeviceIdType.MESH
F32 = jnp.float32
BF16 = jnp.bfloat16
EPS = 1e-6
HIGHEST = lax.Precision.HIGHEST
NT = (((1,), (1,)), ((), ()))
NN = (((1,), (0,)), ((), ()))
RIGHT, LEFT = 0, 1


def step_kernel(
    n_ep,
    ny,
    tok_in, gain_in, routes_in, logits_in, eg_in, eu_in, ed_in, dg_in, du_in, dd_in, mixw_in, og_in,
    out_ref,
    tok, gain, routes, logits, wgu, wdown, dgu, ddown, mixw, og,
    send_a, land_a, xs, ym, yo, yp, ea, eb, send_f, land_f, sq_send, sq_land,
    in_sem, as_sem, ar_sem, bs_sem, br_sem, ds_sem, dr_sem, ps_sem, pr_sem, es_sem, er_sem,
    fs_sem, fr_sem, gs_sem, gr_sem,
):
    n_tp = 2 * ny
    half = n_ep // 2
    group = 4 * half
    ep = lax.axis_index("ep")
    tp = lax.axis_index("tp")
    y = tp // 2
    par = lax.rem(tp, 2)
    width = 256 * n_tp
    x_lo = group + 16
    y_lo = group + 8
    x_rows = (pl.ds(0, group + 16), pl.ds(x_lo, group))
    y_rows = (pl.ds(0, group + 8), pl.ds(y_lo, group))

    bar = pltpu.get_barrier_semaphore()

    def greet_ep(i, _):
        pl.semaphore_signal(bar, inc=1, device_id=(lax.rem(ep + i, n_ep), tp), device_id_type=MESH)
        return 0

    def greet_tp(i, _):
        pl.semaphore_signal(bar, inc=1, device_id=(ep, lax.rem(tp + i, n_tp)), device_id_type=MESH)
        return 0

    lax.fori_loop(1, n_ep, greet_ep, 0)
    lax.fori_loop(1, n_tp, greet_tp, 0)

    loads = [
        pltpu.make_async_copy(src, dst, in_sem.at[i])
        for i, (src, dst) in enumerate(
            [
                (tok_in, tok), (routes_in, routes), (logits_in, logits), (gain_in, gain), (mixw_in, mixw), (og_in, og),
                (eg_in, wgu.at[:, pl.ds(0, 64), :]), (eu_in, wgu.at[:, pl.ds(64, 64), :]),
                (dg_in, dgu.at[pl.ds(0, 64), :]), (du_in, dgu.at[pl.ds(64, 64), :]),
                (ed_in, wdown), (dd_in, ddown),
            ]
        )
    ]
    for load in loads:
        load.start()
    for load in loads[:3]:
        load.wait()

    lanes = 8 * n_ep
    eye = lax.broadcasted_iota(jnp.int32, (8, 8), 0) == lax.broadcasted_iota(jnp.int32, (8, 8), 1)

    def column(v):
        c = jnp.sum(jnp.where(eye, v, 0.0), axis=1, keepdims=True)
        return jnp.concatenate([c, c], axis=0)

    named = routes[...].astype(F32)
    first, second = column(named[0:1]), column(named[1:2])
    lg = logits[...]
    top = jnp.maximum(lg[0:1], lg[1:2])
    w0, w1 = jnp.exp(lg[0:1] - top), jnp.exp(lg[1:2] - top)
    whole = w0 + w1
    w0, w1 = column(w0 / whole), column(w1 / whole)
    lane = lax.broadcasted_iota(jnp.int32, (16, lanes), 1)
    row = lax.broadcasted_iota(jnp.int32, (16, lanes), 0)
    expert = (lane >> 2).astype(F32)
    hit0 = expert == first
    hit = jnp.where(hit0 | (expert == second), 1.0, 0.0)
    a = lax.broadcasted_iota(jnp.int32, (16, 16), 0)
    b = lax.broadcasted_iota(jnp.int32, (16, 16), 1)
    earlier = jnp.where(((a >> 3) == (b >> 3)) & ((b & 7) < (a & 7)), 1.0, 0.0)
    rank = lax.dot_general(earlier, hit, NN, preferred_element_type=F32)
    placed = (hit > 0.5) & (rank == ((lane >> 1) & 1).astype(F32)) & ((lane & 1) == (row >> 3))
    place = jnp.where(placed, 1.0, 0.0)
    weigh = jnp.where(placed, jnp.where(hit0, w0, w1), 0.0)
    mine = tok[...].astype(F32)
    halves = jnp.concatenate([mine[:, :128], mine[:, 128:]], axis=0)
    send_a[...] = lax.dot_general(
        jnp.transpose(place).astype(BF16), halves.astype(BF16), NN, preferred_element_type=F32
    )
    pl.semaphore_wait(bar, n_ep + n_tp - 2)

    block = pl.multiple_of(8 * ep, 8)

    def to_peer(src, dst, s_sem, r_sem, peer):
        return pltpu.make_async_remote_copy(
            src_ref=src.at[pl.ds(pl.multiple_of(8 * peer, 8), 8), :],
            dst_ref=dst.at[pl.ds(block, 8), :],
            send_sem=s_sem.at[peer],
            recv_sem=r_sem.at[ep],
            device_id=(peer, tp),
            device_id_type=MESH,
        )

    def from_peer(src, dst, s_sem, r_sem, peer):
        return pltpu.make_async_remote_copy(
            src_ref=src.at[pl.ds(block, 8), :],
            dst_ref=dst.at[pl.ds(pl.multiple_of(8 * peer, 8), 8), :],
            send_sem=s_sem.at[peer],
            recv_sem=r_sem.at[peer],
            device_id=(peer, tp),
            device_id_type=MESH,
        )

    def send_one(i, _):
        to_peer(send_a, land_a, as_sem, ar_sem, lax.rem(ep + i, n_ep)).start()
        return 0

    lax.fori_loop(1, n_ep, send_one, 0)
    land_a[pl.ds(block, 8), :] = send_a[pl.ds(block, 8), :]
    own16 = jnp.concatenate([mine, jnp.zeros_like(mine)], axis=0).astype(BF16)
    xs[tp, pl.ds(group, 16), :] = own16

    def wait_one(i, _):
        from_peer(send_a, land_a, as_sem, ar_sem, lax.rem(ep + i, n_ep)).wait_recv()
        return 0

    lax.fori_loop(1, n_ep, wait_one, 0)
    for part in range(2):
        for j in range(8):
            xs[tp, pl.ds((x_lo if part else 0) + (j // 2) * half, half), pl.ds((j % 2) * 128, 128)] = land_a[
                pl.ds(part * half * 8 + j, half, stride=8), :
            ].astype(BF16)

    right = (ep, lax.rem(y + 1, ny) * 2 + par)
    left = (ep, lax.rem(y + ny - 1, ny) * 2 + par)
    partner = (ep, y * 2 + (1 - par))
    far = ny // 2

    def slice_of(delta, parity):
        return lax.rem(y + delta, ny) * 2 + parity

    def ring_x(way, q, part, sending):
        age = q - 1 if sending else q
        delta = (ny - age) % ny if way == RIGHT else age % ny
        ref = xs.at[slice_of(delta, par), x_rows[part], :]
        return pltpu.make_async_remote_copy(
            src_ref=ref, dst_ref=ref, send_sem=bs_sem.at[way, q, part], recv_sem=br_sem.at[way, q, part],
            device_id=right if way == RIGHT else left, device_id_type=MESH,
        )

    def pair_x(delta, part, parity):
        ref = xs.at[slice_of(delta, parity), x_rows[part], :]
        return pltpu.make_async_remote_copy(
            src_ref=ref, dst_ref=ref, send_sem=ds_sem.at[delta, part], recv_sem=dr_sem.at[delta, part],
            device_id=partner, device_id_type=MESH,
        )

    sent = []

    def start(copy):
        copy.start()
        sent.append(copy)

    for part in (0, 1):
        start(ring_x(RIGHT, 1, part, True))
        start(ring_x(LEFT, 1, 1 - part, True))
    for part in (0, 1):
        start(pair_x(0, part, par))
    for q in range(1, far + 1):
        for turn in (0, 1):
            for way in (RIGHT, LEFT):
                part = turn if way == RIGHT else 1 - turn
                if q == far and turn:
                    continue
                ring_x(way, q, part, False).wait_recv()
                if q < far - 1 or (q == far - 1 and turn == 0):
                    start(ring_x(way, q + 1, part, True))
                start(pair_x((ny - q) % ny if way == RIGHT else q % ny, part, par))
    for load in loads[3:]:
        load.wait()
    for delta in range(ny):
        for part in (0, 1):
            pair_x(delta, part, 1 - par).wait_recv()

    n_rows = 2 * group + 16

    def squares(k, acc):
        v = xs[k].astype(F32)
        lo, hi = v[:, :128], v[:, 128:]
        return acc + (lo * lo + hi * hi)

    total = lax.fori_loop(0, n_tp, squares, jnp.zeros((n_rows, 128), F32))
    scale = lax.rsqrt(jnp.sum(total, axis=1, keepdims=True) / width + EPS)
    side = 2 * half

    def project(k, carry):
        e0, e1, dn, mg = carry
        v = xs[k].astype(F32) * scale
        lo = v[:, :128] * gain[pl.ds(2 * k, 1), :]
        hi = v[:, 128:] * gain[pl.ds(2 * k + 1, 1), :]
        nrm = jnp.concatenate([lo, hi], axis=1).astype(BF16)
        cols = pl.ds(pl.multiple_of(k * 256, 256), 256)
        r0 = jnp.concatenate([nrm[0:side], nrm[x_lo : x_lo + side]], axis=0)
        r1 = jnp.concatenate([nrm[side : 2 * side], nrm[x_lo + side : x_lo + 2 * side]], axis=0)
        rd = nrm[group : group + 16]
        e0 = e0 + lax.dot_general(r0, wgu[0, :, cols], NT, preferred_element_type=F32)
        e1 = e1 + lax.dot_general(r1, wgu[1, :, cols], NT, preferred_element_type=F32)
        dn = dn + lax.dot_general(rd, dgu[:, cols], NT, preferred_element_type=F32)
        d32 = rd.astype(F32)
        mg = mg + d32[0:8, :128] * mixw[pl.ds(2 * k, 1), :] + d32[0:8, 128:] * mixw[pl.ds(2 * k + 1, 1), :]
        return e0, e1, dn, mg

    e0, e1, dn, mg = lax.fori_loop(
        0, n_tp, project,
        (
            jnp.zeros((2 * side, 128), F32), jnp.zeros((2 * side, 128), F32), jnp.zeros((16, 128), F32),
            jnp.zeros((8, 128), F32),
        ),
    )

    def hidden(v):
        g = v[:, :64]
        return (g / (1.0 + jnp.exp(-g)) * v[:, 64:]).astype(BF16)

    h0, h1, hd = hidden(e0), hidden(e1), hidden(dn)
    mix_gate = 1.0 / (1.0 + jnp.exp(-jnp.sum(mg, axis=1, keepdims=True)))

    def down(i, parity):
        delta = lax.rem(far + i, ny)
        cols = pl.ds(pl.multiple_of(slice_of(delta, parity) * 256, 256), 256)
        o0 = lax.dot_general(h0, wdown[0, :, cols], NN, preferred_element_type=F32)
        o1 = lax.dot_general(h1, wdown[1, :, cols], NN, preferred_element_type=F32)
        od = lax.dot_general(hd, ddown[:, cols], NN, preferred_element_type=F32)
        return delta, o0, o1, od

    def fill(ref, delta, o0, o1, od):
        ref[delta, pl.ds(0, side), :] = o0[:side]
        ref[delta, pl.ds(side, side), :] = o1[:side]
        ref[delta, pl.ds(group, 8), :] = od[:8]
        ref[delta, pl.ds(y_lo, side), :] = o0[side:]
        ref[delta, pl.ds(y_lo + side, side), :] = o1[side:]

    def pair_y(delta):
        return pltpu.make_async_remote_copy(
            src_ref=yo.at[delta], dst_ref=yp.at[delta], send_sem=ps_sem.at[delta], recv_sem=pr_sem.at[delta],
            device_id=partner, device_id_type=MESH,
        )

    def produce(i, _):
        fill(yo, *down(i, 1 - par))
        pair_y(lax.rem(far + i, ny)).start()
        fill(ym, *down(i, par))
        return 0

    lax.fori_loop(0, ny, produce, 0)

    lands = (ea, eb)

    def ring_y(way, q, part):
        delta = q % ny if way == RIGHT else (ny - q) % ny
        return pltpu.make_async_remote_copy(
            src_ref=ym.at[delta, y_rows[part], :], dst_ref=lands[part].at[way, q],
            send_sem=es_sem.at[way, q, part], recv_sem=er_sem.at[way, q, part],
            device_id=right if way == RIGHT else left, device_id_type=MESH,
        )

    def gather(delta, part, came):
        v = ym[delta, y_rows[part], :] + yp[delta, y_rows[part], :]
        for way, q in came:
            ring_y(way, q, part).wait_recv()
            v = v + lands[part][way, q]
        ym[delta, y_rows[part], :] = v

    for q in range(far, 0, -1):
        for delta in sorted({q % ny, (ny - q) % ny}):
            pair_y(delta).wait_recv()
        for turn in (1, 0) if q < far else (0,):
            for way in (RIGHT, LEFT):
                part = turn if way == RIGHT else 1 - turn
                delta = q % ny if way == RIGHT else (ny - q) % ny
                have = q + 1 < far or (q + 1 == far and turn == 0)
                gather(delta, part, [(way, q + 1)] if have else [])
                start(ring_y(way, q, part))
    pair_y(0).wait_recv()

    for part in (1, 0):
        gather(0, part, [(RIGHT, 1), (LEFT, 1)])
        lo = y_lo if part else 0
        for j in range(8):
            send_f[pl.ds(part * half * 8 + j, half, stride=8), :] = ym[
                0, pl.ds(lo + (j // 2) * half, half), pl.ds((j % 2) * 128, 128)
            ]

        def send_back(i, _, part=part):
            peer = part * half + lax.rem(ep + i, half)

            @pl.when(peer != ep)
            def _():
                to_peer(send_f, land_f, fs_sem, fr_sem, peer).start()

            return 0

        lax.fori_loop(0, half, send_back, 0)
    land_f[pl.ds(block, 8), :] = send_f[pl.ds(block, 8), :]
    dense = ym[0, pl.ds(group, 8), :]
    dense16 = jnp.concatenate([dense[:, :128] * mix_gate, dense[:, 128:] * mix_gate], axis=0)

    def wait_back(i, _):
        from_peer(send_f, land_f, fs_sem, fr_sem, lax.rem(ep + i, n_ep)).wait_recv()
        return 0

    lax.fori_loop(1, n_ep, wait_back, 0)
    mixed = lax.dot_general(weigh, land_f[...], NN, precision=HIGHEST, preferred_element_type=F32) + dense16

    part_sq = jnp.sum(mixed[:8] * mixed[:8] + mixed[8:] * mixed[8:], axis=1, keepdims=True)
    diag = lax.broadcasted_iota(jnp.int32, (8, 128), 0) == lax.broadcasted_iota(jnp.int32, (8, 128), 1)
    sq_row = jnp.sum(jnp.where(diag, part_sq, 0.0), axis=0, keepdims=True)
    sq_send[...] = sq_row
    sq_land[tp] = sq_row

    def sq_copy(to, at):
        return pltpu.make_async_remote_copy(
            src_ref=sq_send, dst_ref=sq_land.at[at], send_sem=gs_sem.at[to], recv_sem=gr_sem.at[at],
            device_id=(ep, to), device_id_type=MESH,
        )

    def sq_start(i, _):
        sq_copy(lax.rem(tp + i, n_tp), tp).start()
        return 0

    def sq_wait(i, _):
        other = lax.rem(tp + i, n_tp)
        sq_copy(other, other).wait_recv()
        return 0

    lax.fori_loop(1, n_tp, sq_start, 0)
    lax.fori_loop(1, n_tp, sq_wait, 0)
    whole_sq = jnp.sum(jnp.sum(sq_land[...], axis=0), axis=0, keepdims=True)
    sq_col = jnp.sum(jnp.where(diag, whole_sq, 0.0), axis=1, keepdims=True)
    norm = lax.rsqrt(sq_col / width + EPS)
    out_ref[:, pl.ds(0, 128)] = (mixed[:8] * norm * og[0:1, :]).astype(BF16)
    out_ref[:, pl.ds(128, 128)] = (mixed[8:] * norm * og[1:2, :]).astype(BF16)

    for copy in sent:
        copy.wait_send()

    def drain_ep(i, _):
        peer = lax.rem(ep + i, n_ep)
        to_peer(send_a, land_a, as_sem, ar_sem, peer).wait_send()
        to_peer(send_f, land_f, fs_sem, fr_sem, peer).wait_send()
        return 0

    def drain_tp(i, _):
        sq_copy(lax.rem(tp + i, n_tp), tp).wait_send()
        return 0

    def drain_pair(i, _):
        pair_y(i).wait_send()
        return 0

    lax.fori_loop(1, n_ep, drain_ep, 0)
    lax.fori_loop(1, n_tp, drain_tp, 0)
    lax.fori_loop(0, ny, drain_pair, 0)


def local(
    n_ep, n_tp,
    tokens, norm_gain, route_experts, route_logits, expert_gate, expert_up, expert_down,
    dense_gate, dense_up, dense_down, mix_weight, out_gain,
):
    ny = n_tp // 2
    half = n_ep // 2
    group = 4 * half
    width = n_tp * 256
    far = ny // 2
    vmem, dma = pltpu.VMEM, pltpu.SemaphoreType.DMA
    args = (
        tokens,
        norm_gain.reshape(width // 128, 128),
        route_experts.T,
        route_logits.T,
        jnp.swapaxes(expert_gate, 1, 2),
        jnp.swapaxes(expert_up, 1, 2),
        expert_down,
        dense_gate.T,
        dense_up.T,
        dense_down,
        mix_weight.reshape(width // 128, 128),
        out_gain.reshape(2, 128),
    )
    return pl.pallas_call(
        functools.partial(step_kernel, n_ep, ny),
        out_shape=jax.ShapeDtypeStruct((8, 256), BF16),
        in_specs=[pl.BlockSpec(memory_space=pl.ANY)] * len(args),
        out_specs=pl.BlockSpec(memory_space=pltpu.VMEM),
        scratch_shapes=[
            vmem((8, 256), BF16), vmem((width // 128, 128), F32), vmem((2, 8), jnp.int32), vmem((2, 8), F32),
            vmem((2, 128, width), BF16), vmem((2, 64, width), BF16), vmem((128, width), BF16), vmem((64, width), BF16),
            vmem((width // 128, 128), F32), vmem((2, 128), F32),
            vmem((8 * n_ep, 128), F32), vmem((8 * n_ep, 128), F32),
            vmem((n_tp, 2 * group + 16, 256), BF16),
            vmem((ny, 2 * group + 8, 256), F32), vmem((ny, 2 * group + 8, 256), F32), vmem((ny, 2 * group + 8, 256), F32),
            vmem((2, far + 1, group + 8, 256), F32), vmem((2, far + 1, group, 256), F32),
            vmem((8 * n_ep, 128), F32), vmem((8 * n_ep, 128), F32),
            vmem((1, 128), F32), vmem((n_tp, 1, 128), F32),
            dma((12,)), dma((n_ep,)), dma((n_ep,)),
            dma((2, far + 1, 2)), dma((2, far + 1, 2)), dma((ny, 2)), dma((ny, 2)), dma((ny,)), dma((ny,)),
            dma((2, far + 1, 2)), dma((2, far + 1, 2)),
            dma((n_ep,)), dma((n_ep,)), dma((n_tp,)), dma((n_tp,)),
        ],
        compiler_params=pltpu.CompilerParams(collective_id=0, has_side_effects=True),
        name="step",
    )(*args)


def solution(mesh):
    tp = "tp"
    in_specs = (
        P("ep", tp), P(), P("ep", None), P("ep", None),
        P("ep", None, tp), P("ep", None, tp), P("ep", tp, None),
        P(None, tp), P(None, tp), P(tp, None), P(), P(tp),
    )
    return jax.shard_map(
        functools.partial(local, mesh.shape["ep"], mesh.shape["tp"]),
        mesh=mesh, in_specs=in_specs, out_specs=P("ep", tp), check_vma=False,
    )
```
